32 devices in a mesh: sp: 8 (over z, x), tp: 4 (over y, core).
Axes of the slice: x: 2, y: 2, z: 4, core: 2. Of those that a mesh axis runs over, the one named last changes fastest.
Arguments:
- residual: bfloat16 [4096, 2048], P(('sp', 'tp')), may hold values from -6 to 6
- conv_value: bfloat16 [4096, 1024], P('sp', 'tp'), may hold values from -6 to 6
- conv_gate: bfloat16 [4096, 1024], P('sp', 'tp'), may hold values from -9 to 9
- segments: int32 [4096], P('sp'), may hold values from 0 to 3, never falling along the last dimension, each value on 1 to 2048 neighbouring positions
- conv_weight: float32 [31, 1024], P(None, 'tp'), may hold values from -1 to 1
- norm_gain: float32 [1024], P('tp'), may hold values from 0.1 to 1.9
- norm_shift: float32 [1024], P('tp'), may hold values from -3 to 3
- out_weight: bfloat16 [1024, 2048], replicated, may hold values from -0.1875 to 0.1875
- ffn_gain: float32 [2048], replicated, may hold values from 0.1 to 1.9
- routes: int32 [4096, 2], P('sp'), may hold values from 0 to 7, all different within a row; in each aligned block of 128 rows (0 to 127, 128 to 255, ...) at most 64 rows name the same one
- route_weights: float32 [4096, 2], P('sp'), may hold values from 0.2 to 1
- w_gate: bfloat16 [8, 2048, 1024], P('sp', None, 'tp'), may hold values from -0.125 to 0.125
- w_up: bfloat16 [8, 2048, 1024], P('sp', None, 'tp'), may hold values from -0.125 to 0.125
- w_down: bfloat16 [8, 1024, 2048], P('sp', 'tp'), may hold values from -0.1875 to 0.1875
Outputs:
- layer_out: bfloat16 [4096, 2048], P(('sp', 'tp'))
The draws below stay inside these ranges and needn't reach their ends.
Inputs may be any that keep to these rules, and one draw needn't show every extreme that they name: `routes`: within the rows of one device (aligned blocks of 512 / 4 rows), no expert is named more than 64 times; the two experts of a row differ. `segments`: document numbers never fall along the sequence.
All inputs are finite; a program needn't handle non-finite values.
Results may differ from the reference program's by a relative error of at most 0.007.
Values may be sent and summed in bfloat16 or wider, within the bound.
A program may use at most 128 MiB of HBM per device.

```python
import math
import jax
import jax.numpy as jnp
import numpy as np
from jax import lax

D = 2048
DC = 1024
FF = 1024
CONV_WIDTH = 31
CONV_GROUPS = 8
TOPK = 2
TOK_DEV = 512
TOKENS = 4096
EXPERTS = 8
CAP = 64
N_SP = 8
N_TP = 4


def steps_of(stream_key, shape, cuts, low, largest):
    level = 1.0
    for dim, shards_of in cuts:
        heights = jax.random.uniform(jax.random.fold_in(jax.random.fold_in(stream_key, 6), dim), (shards_of,), jnp.float32, low / len(cuts), largest / len(cuts))
        level = level * jnp.repeat(jnp.exp(heights), shape[dim] // shards_of).reshape((-1,) + (1,) * (len(shape) - 1 - dim))
    return level


def profile(amount, total, bound, slope):
    weights = [(1 << 20) // math.isqrt(grade ** slope) + 1 for grade in range(2, amount + 1)]
    spare, given = total - bound - (amount - 1), [1] * (amount - 1)
    while spare > 0:
        candidates = [i for i in range(amount - 1) if given[i] < bound]
        pool, left = sum([weights[i] for i in candidates]), spare
        for i in candidates:
            more = min(bound - given[i], max(1, left * weights[i] // pool), spare)
            given[i] = given[i] + more
            spare = spare - more
    return np.array([bound] + given)


def uneven(key, number_of, total, most, lean):
    if number_of == 2:
        one = jax.random.randint(key, (), max(1, total - most), min(most, total - 1) + 1)
        return jnp.stack([one, total - one])
    sizes = jnp.asarray(profile(number_of, total, most, lean), jnp.int32)
    couples = (number_of - 1) // 2
    donor, sink = sizes[1:1 + 2 * couples:2], sizes[2:2 + 2 * couples:2]
    margin = jnp.minimum(donor - 1, most - sink)
    shifted = jax.random.randint(jax.random.fold_in(key, 1), (couples,), 0, 1 << 20) % (margin + 1)
    sizes = sizes.at[1:1 + 2 * couples:2].set(donor - shifted).at[2:2 + 2 * couples:2].set(sink + shifted)
    return sizes[jax.random.permutation(jax.random.fold_in(key, 2), number_of)]


def assign_block(key, own, number, rows, count, top, most, lean):
    sequence = jax.random.permutation(key, count)
    crowded, usual = portions_of(count, rows * top, most, lean, True), portions_of(count, rows * top, most, lean, False)
    places = jnp.arange(count)

    def named(tallies, turn):
        used = int((tallies > 0).sum())
        fixed = max(1, used // 4)
        passed = fixed + (places - fixed + turn * (used - fixed)) % max(1, count - fixed)
        return jnp.zeros((count,), jnp.int32).at[sequence[jnp.where(places < fixed, places, passed)]].set(jnp.asarray(tallies, jnp.int32))

    tallies = jnp.where(number % 4 == 0, named(crowded, number // 4), named(usual, number - number // 4 - 1))
    mixed = jax.random.permutation(jax.random.fold_in(own, 3), count)
    donor, taker = mixed[0:count // 2 * 2:2], mixed[1:count // 2 * 2:2]
    slack = jnp.minimum(tallies[donor] - 1, most - tallies[taker]) // 2
    slack = jnp.where((donor == sequence[0]) | (taker == sequence[0]) | (tallies[taker] == 0), 0, jnp.maximum(slack, 0))
    passed = jax.random.randint(jax.random.fold_in(own, 4), (count // 2,), 0, 1 << 20) % (slack + 1)
    tallies = tallies.at[donor].add(-passed).at[taker].add(passed)
    items = jnp.searchsorted(jnp.cumsum(tallies), jnp.arange(rows * top), side="right").astype(jnp.int32)
    table = items.reshape(top, rows).T
    table = table[jax.random.permutation(jax.random.fold_in(own, 1), rows)]
    turn = jax.random.randint(jax.random.fold_in(own, 2), (rows, 1), 0, top)
    return jnp.take_along_axis(table, (jnp.arange(top)[None, :] + turn) % top, axis=1)


def portions_of(count, total, limit, slope, full):
    loads = [(1 << 20) // math.isqrt(standing ** slope) + 1 for standing in range(1, count + 1)]
    largest = limit if full else min(limit, max(-(-total // count), total * loads[0] // sum(loads)))
    least = 1 if total - largest >= count - 1 else 0
    holding, rest = [largest] + [least] * (count - 1), total - largest - least * (count - 1)
    while rest > 0:
        movable = [i for i in range(1, count) if holding[i] < largest] or [i for i in range(1, count) if holding[i] < limit]
        pool, budget = sum([loads[i] for i in movable]), rest
        for i in movable:
            addition = min(limit - holding[i], max(1, budget * loads[i] // pool), rest)
            holding[i] = holding[i] + addition
            rest = rest - addition
    return np.array(holding)


def gaussian(stream_key, extent, scale, most, cuts=(), kind=jnp.bfloat16):
    result = scale * jax.random.normal(stream_key, extent, jnp.float32)
    if cuts:
        result = result * steps_of(stream_key, extent, cuts, -0.22, 0.18)
    return jnp.clip(result, -most, most).astype(kind)


def setup_inputs(seed: int = 0) -> dict:
    arg_keys = jax.random.split(jax.random.key(seed), 15)
    residual = gaussian(arg_keys[0], (TOKENS, D), 1.0, 6.0, ((0, 32),))
    conv_value = gaussian(arg_keys[1], (TOKENS, DC), 1.0, 6.0, ((0, 8), (1, 4)))
    conv_gate = gaussian(arg_keys[2], (TOKENS, DC), 1.5, 9.0, ((0, 8), (1, 4)))
    segments = jnp.searchsorted(jnp.cumsum(uneven(arg_keys[3], N_SP // 2, TOKENS, 4 * TOK_DEV, 0)), jnp.arange(TOKENS), side="right").astype(jnp.int32)
    conv_weight = gaussian(arg_keys[4], (CONV_WIDTH, DC), CONV_WIDTH ** -0.5, 1.0, ((1, 4),), jnp.float32)
    norm_gain = jnp.clip(1.0 + 0.18 * jax.random.normal(arg_keys[5], (DC,), jnp.float32), 0.1, 1.9)
    norm_shift = gaussian(arg_keys[6], (DC,), 0.5, 3.0, ((0, 4),), jnp.float32)
    out_weight = gaussian(arg_keys[7], (DC, D), DC ** -0.5, 0.1875)
    ffn_gain = jnp.clip(1.0 + 0.18 * jax.random.normal(arg_keys[8], (D,), jnp.float32), 0.1, 1.9)
    routes_keys = jax.random.split(jax.random.fold_in(arg_keys[9], 1), TOKENS // (TOK_DEV // N_TP))
    routes_turns = jax.random.permutation(jax.random.fold_in(arg_keys[9], 3), TOKENS // (TOK_DEV // N_TP))
    routes = jax.vmap(lambda own, number: assign_block(jax.random.fold_in(arg_keys[9], 2), own, number, TOK_DEV // N_TP, EXPERTS, TOPK, CAP, 2))(routes_keys, routes_turns).reshape((TOKENS, TOPK))
    route_weights = jnp.clip(0.2 + 0.8 * jax.random.uniform(arg_keys[10], (TOKENS, TOPK), jnp.float32) ** steps_of(arg_keys[10], (TOKENS, TOPK), ((0, 8),), -0.2, 0.2), 0.2, 1.0)
    w_gate = gaussian(arg_keys[11], (EXPERTS, D, FF), D ** -0.5, 0.125, ((0, 8), (2, 4)))
    w_up = gaussian(arg_keys[12], (EXPERTS, D, FF), D ** -0.5, 0.125, ((0, 8), (2, 4)))
    w_down = gaussian(arg_keys[13], (EXPERTS, FF, D), FF ** -0.5, 0.1875, ((0, 8), (1, 4)))
    return dict(residual=residual, conv_value=conv_value, conv_gate=conv_gate, segments=segments, conv_weight=conv_weight, norm_gain=norm_gain, norm_shift=norm_shift, out_weight=out_weight, ffn_gain=ffn_gain, routes=routes, route_weights=route_weights, w_gate=w_gate, w_up=w_up, w_down=w_down)


def reference(residual, conv_value, conv_gate, segments, conv_weight, norm_gain, norm_shift, out_weight, ffn_gain, routes, route_weights, w_gate, w_up, w_down):
    gated = (conv_value.astype(jnp.float32) * jax.nn.sigmoid(conv_gate.astype(jnp.float32))).astype(jnp.bfloat16)
    reach = CONV_WIDTH - 1
    padded = jnp.concatenate([jnp.zeros((reach, DC), jnp.bfloat16), gated], 0).astype(jnp.float32)
    seg_padded = jnp.concatenate([jnp.full((reach,), -1, jnp.int32), segments.astype(jnp.int32)], 0)
    convolved = jnp.zeros((TOKENS, DC), jnp.float32)
    for offset in range(CONV_WIDTH):
        same_doc = (seg_padded[offset:offset + TOKENS] == segments)[:, None]
        convolved = convolved + jnp.where(same_doc, padded[offset:offset + TOKENS] * conv_weight[offset], 0.0)
    grouped = convolved.reshape(TOKENS, CONV_GROUPS, DC // CONV_GROUPS)
    group_mean = lax.optimization_barrier(jnp.mean(grouped, axis=-1, keepdims=True))
    group_var = lax.optimization_barrier(jnp.mean(jnp.square(grouped - group_mean), axis=-1, keepdims=True))
    scaled = ((grouped - group_mean) * lax.rsqrt(group_var + 1e-05)).reshape(TOKENS, DC) * norm_gain + norm_shift
    conv_out = jax.nn.silu(scaled).astype(jnp.bfloat16)
    mixed = jnp.dot(conv_out, out_weight, preferred_element_type=jnp.float32).astype(jnp.bfloat16)
    stream = residual.astype(jnp.float32) + lax.optimization_barrier(mixed).astype(jnp.float32)
    normed = (stream * lax.rsqrt(lax.optimization_barrier(jnp.mean(stream * stream, axis=-1, keepdims=True)) + 1e-06) * ffn_gain).astype(jnp.bfloat16)
    rows_dev = TOK_DEV // N_TP
    blocks = TOKENS // rows_dev
    route_pairs = routes.reshape(blocks, rows_dev * TOPK)
    onehot = (route_pairs[..., None] == jnp.arange(EXPERTS, dtype=jnp.int32)).astype(jnp.int32)
    slot_rank = lax.optimization_barrier(jnp.sum((jnp.cumsum(onehot, axis=1) - onehot) * onehot, axis=2)).reshape(TOKENS, TOPK)
    token_id = jnp.broadcast_to(jnp.arange(TOKENS, dtype=jnp.int32)[:, None], (TOKENS, TOPK))
    block_id = token_id // rows_dev
    owners = jnp.full((EXPERTS, blocks, CAP), TOKENS, jnp.int32).at[routes, block_id, slot_rank].set(token_id)
    weight_table = jnp.zeros((EXPERTS, blocks, CAP), jnp.float32).at[routes, block_id, slot_rank].set(route_weights)
    rows_pad = jnp.concatenate([normed, jnp.zeros((1, D), jnp.bfloat16)], 0)

    def one_expert(totals, inputs):
        gate_w, up_w, down_w, expert_owners, expert_weights = inputs
        row_index = expert_owners.reshape(-1)
        picked = rows_pad[row_index]
        gate_act = jnp.dot(picked, gate_w, preferred_element_type=jnp.float32)
        up_act = jnp.dot(picked, up_w, preferred_element_type=jnp.float32)
        hidden = (jax.nn.silu(gate_act) * up_act).astype(jnp.bfloat16)
        summed = jnp.dot(hidden, down_w, preferred_element_type=jnp.float32)
        expert_out = lax.optimization_barrier(summed.astype(jnp.bfloat16)).astype(jnp.float32)
        totals = totals.at[row_index].add(expert_weights.reshape(-1)[:, None] * expert_out)
        return (totals, None)
    totals, _ = lax.scan(one_expert, jnp.zeros((TOKENS + 1, D), jnp.float32), (w_gate, w_up, w_down, owners, weight_table))
    return (stream + totals[:TOKENS]).astype(jnp.bfloat16)
```

```python
import jax
import jax.numpy as jnp
from jax import lax
from jax.sharding import PartitionSpec as P

DC = 1024
CONV_GROUPS = 8


def passed_along(value, axis, steps):
    count = lax.axis_size(axis)
    initial, last = (max(0, -steps), min(count, count - steps))
    return lax.ppermute(value, axis, [(source, source + steps) for source in range(initial, last)])


def slot_numbers(block_routes, capacity, experts_n):
    route_pairs = block_routes.reshape(block_routes.shape[:-2] + (-1,))
    onehot = (route_pairs[..., None] == jnp.arange(experts_n, dtype=jnp.int32)).astype(jnp.int32)
    slot_rank = jnp.sum((jnp.cumsum(onehot, axis=-2) - onehot) * onehot, axis=-1)
    return (route_pairs * capacity + slot_rank).reshape(block_routes.shape)


def dispatch_matrix(slot_ids, slot_total):
    numbers = jnp.arange(slot_total, dtype=jnp.int32)[:, None, None]
    matches = jnp.any(numbers == slot_ids[..., None, :, :], axis=-1)
    return matches.astype(jnp.bfloat16)


def shards(
    residual,
    conv_value,
    conv_gate,
    segments,
    conv_weight,
    norm_gain,
    norm_shift,
    out_weight,
    ffn_gain,
    routes,
    route_weights,
    w_gate,
    w_up,
    w_down,
):
    tok_dev, local_channels = conv_value.shape
    reach = conv_weight.shape[0] - 1
    whole_gate, whole_up = (
        lax.all_gather(w_gate[0], "tp", axis=1, tiled=True),
        lax.all_gather(w_up[0], "tp", axis=1, tiled=True),
    )
    whole_down = lax.all_gather(w_down[0], "tp", axis=0, tiled=True)
    gated = (conv_value.astype(jnp.float32) * jax.nn.sigmoid(conv_gate.astype(jnp.float32))).astype(
        jnp.bfloat16
    )
    rim_prev, seg_prev = passed_along(
        (gated[tok_dev - reach :], segments[tok_dev - reach :]), "sp", 1
    )
    extended = jnp.concatenate([rim_prev, gated], 0).astype(jnp.float32)
    seg_ext = jnp.concatenate([seg_prev, segments], 0)
    convolved = jnp.zeros((tok_dev, local_channels), jnp.float32)
    for offset in range(reach + 1):
        same_doc = (seg_ext[offset : offset + tok_dev] == segments)[:, None]
        convolved = convolved + jnp.where(
            same_doc, extended[offset : offset + tok_dev] * conv_weight[offset], 0.0
        )
    group_size = DC // CONV_GROUPS
    grouped = convolved.reshape(tok_dev, local_channels // group_size, group_size)
    group_mean = jnp.mean(grouped, axis=-1, keepdims=True)
    group_var = jnp.mean(jnp.square(grouped - group_mean), axis=-1, keepdims=True)
    scaled = ((grouped - group_mean) * lax.rsqrt(group_var + 1e-05)).reshape(
        tok_dev, local_channels
    ) * norm_gain + norm_shift
    conv_out = jax.nn.silu(scaled).astype(jnp.bfloat16)
    columns = lax.axis_size("tp")
    column = lax.axis_index("tp")
    rows_own = tok_dev // columns
    own_conv = lax.all_to_all(conv_out, "tp", split_axis=0, concat_axis=1, tiled=True)
    mixed = jnp.dot(own_conv, out_weight, preferred_element_type=jnp.float32)
    stream = residual.astype(jnp.float32) + lax.optimization_barrier(
        mixed.astype(jnp.bfloat16)
    ).astype(jnp.float32)
    normed = (
        stream * lax.rsqrt(jnp.mean(stream * stream, axis=-1, keepdims=True) + 1e-06) * ffn_gain
    ).astype(jnp.bfloat16)
    experts_n = lax.axis_size("sp")
    top_count = routes.shape[1]
    model_width = normed.shape[1]
    capacity = max(2, 2 * tok_dev * top_count // (columns * experts_n))
    slot_total = experts_n * capacity
    own_routes = lax.dynamic_slice_in_dim(routes, column * rows_own, rows_own, 0)
    own_weights = lax.dynamic_slice_in_dim(route_weights, column * rows_own, rows_own, 0)
    own_slots = slot_numbers(own_routes, capacity, experts_n)
    routing_table = dispatch_matrix(own_slots, slot_total)
    outgoing = jnp.dot(routing_table, normed, preferred_element_type=jnp.float32).astype(
        jnp.bfloat16
    )
    outgoing = outgoing.reshape(experts_n, capacity, model_width)
    arrived = lax.all_to_all(outgoing, "sp", split_axis=0, concat_axis=1, tiled=True).reshape(
        slot_total, model_width
    )
    gate_act = jnp.dot(arrived, whole_gate, preferred_element_type=jnp.float32)
    up_act = jnp.dot(arrived, whole_up, preferred_element_type=jnp.float32)
    hidden = (jax.nn.silu(gate_act) * up_act).astype(jnp.bfloat16)
    summed = jnp.dot(hidden, whole_down, preferred_element_type=jnp.float32)
    expert_out = summed.astype(jnp.bfloat16).reshape(experts_n, capacity, model_width)
    returned = lax.all_to_all(expert_out, "sp", split_axis=0, concat_axis=0, tiled=True).reshape(
        slot_total, model_width
    )
    combined = stream
    for member in range(top_count):
        chosen = jnp.take(returned, own_slots[:, member], axis=0).astype(jnp.float32)
        combined = combined + own_weights[:, member : member + 1] * chosen
    return combined.astype(jnp.bfloat16)


def solution(mesh):
    return jax.shard_map(
        shards,
        mesh=mesh,
        in_specs=(
            P(("sp", "tp"), None),
            P("sp", "tp"),
            P("sp", "tp"),
            P("sp"),
            P(None, "tp"),
            P("tp"),
            P("tp"),
            P(),
            P(),
            P("sp", None),
            P("sp", None),
            P("sp", None, "tp"),
            P("sp", None, "tp"),
            P("sp", "tp", None),
        ),
        out_specs=P(("sp", "tp"), None),
        check_vma=False,
    )
```

```python
import functools

import jax
import jax.numpy as jnp
from jax import lax
from jax.experimental import pallas as pl
from jax.experimental.pallas import tpu as pltpu
from jax.sharding import PartitionSpec as P

DC = 1024
CONV_GROUPS = 8
MESH = pl.DeviceIdType.MESH
RIM = 32


def passed_along(value, axis, steps):
    count = lax.axis_size(axis)
    initial, last = (max(0, -steps), min(count, count - steps))
    return lax.ppermute(value, axis, [(source, source + steps) for source in range(initial, last)])


def slot_numbers(block_routes, capacity, experts_n):
    route_pairs = block_routes.reshape(block_routes.shape[:-2] + (-1,))
    onehot = (route_pairs[..., None] == jnp.arange(experts_n, dtype=jnp.int32)).astype(jnp.int32)
    slot_rank = jnp.sum((jnp.cumsum(onehot, axis=-2) - onehot) * onehot, axis=-1)
    return (route_pairs * capacity + slot_rank).reshape(block_routes.shape)


def dispatch_matrix(slot_ids, slot_total):
    numbers = jnp.arange(slot_total, dtype=jnp.int32)[:, None, None]
    matches = jnp.any(numbers == slot_ids[..., None, :, :], axis=-1)
    return matches.astype(jnp.bfloat16)


def plain_shards(
    residual,
    conv_value,
    conv_gate,
    segments,
    conv_weight,
    norm_gain,
    norm_shift,
    out_weight,
    ffn_gain,
    routes,
    route_weights,
    w_gate,
    w_up,
    w_down,
):
    tok_dev, local_channels = conv_value.shape
    reach = conv_weight.shape[0] - 1
    whole_gate, whole_up = (
        lax.all_gather(w_gate[0], "tp", axis=1, tiled=True),
        lax.all_gather(w_up[0], "tp", axis=1, tiled=True),
    )
    whole_down = lax.all_gather(w_down[0], "tp", axis=0, tiled=True)
    gated = (conv_value.astype(jnp.float32) * jax.nn.sigmoid(conv_gate.astype(jnp.float32))).astype(
        jnp.bfloat16
    )
    rim_prev, seg_prev = passed_along(
        (gated[tok_dev - reach :], segments[tok_dev - reach :]), "sp", 1
    )
    extended = jnp.concatenate([rim_prev, gated], 0).astype(jnp.float32)
    seg_ext = jnp.concatenate([seg_prev, segments], 0)
    convolved = jnp.zeros((tok_dev, local_channels), jnp.float32)
    for offset in range(reach + 1):
        same_doc = (seg_ext[offset : offset + tok_dev] == segments)[:, None]
        convolved = convolved + jnp.where(
            same_doc, extended[offset : offset + tok_dev] * conv_weight[offset], 0.0
        )
    group_size = DC // CONV_GROUPS
    grouped = convolved.reshape(tok_dev, local_channels // group_size, group_size)
    group_mean = jnp.mean(grouped, axis=-1, keepdims=True)
    group_var = jnp.mean(jnp.square(grouped - group_mean), axis=-1, keepdims=True)
    scaled = ((grouped - group_mean) * lax.rsqrt(group_var + 1e-05)).reshape(
        tok_dev, local_channels
    ) * norm_gain + norm_shift
    conv_out = jax.nn.silu(scaled).astype(jnp.bfloat16)
    columns = lax.axis_size("tp")
    column = lax.axis_index("tp")
    rows_own = tok_dev // columns
    own_conv = lax.all_to_all(conv_out, "tp", split_axis=0, concat_axis=1, tiled=True)
    mixed = jnp.dot(own_conv, out_weight, preferred_element_type=jnp.float32)
    stream = residual.astype(jnp.float32) + lax.optimization_barrier(
        mixed.astype(jnp.bfloat16)
    ).astype(jnp.float32)
    normed = (
        stream * lax.rsqrt(jnp.mean(stream * stream, axis=-1, keepdims=True) + 1e-06) * ffn_gain
    ).astype(jnp.bfloat16)
    experts_n = lax.axis_size("sp")
    top_count = routes.shape[1]
    model_width = normed.shape[1]
    capacity = max(2, 2 * tok_dev * top_count // (columns * experts_n))
    slot_total = experts_n * capacity
    own_routes = lax.dynamic_slice_in_dim(routes, column * rows_own, rows_own, 0)
    own_weights = lax.dynamic_slice_in_dim(route_weights, column * rows_own, rows_own, 0)
    own_slots = slot_numbers(own_routes, capacity, experts_n)
    routing_table = dispatch_matrix(own_slots, slot_total)
    outgoing = jnp.dot(routing_table, normed, preferred_element_type=jnp.float32).astype(
        jnp.bfloat16
    )
    outgoing = outgoing.reshape(experts_n, capacity, model_width)
    arrived = lax.all_to_all(outgoing, "sp", split_axis=0, concat_axis=1, tiled=True).reshape(
        slot_total, model_width
    )
    gate_act = jnp.dot(arrived, whole_gate, preferred_element_type=jnp.float32)
    up_act = jnp.dot(arrived, whole_up, preferred_element_type=jnp.float32)
    hidden = (jax.nn.silu(gate_act) * up_act).astype(jnp.bfloat16)
    summed = jnp.dot(hidden, whole_down, preferred_element_type=jnp.float32)
    expert_out = summed.astype(jnp.bfloat16).reshape(experts_n, capacity, model_width)
    returned = lax.all_to_all(expert_out, "sp", split_axis=0, concat_axis=0, tiled=True).reshape(
        slot_total, model_width
    )
    combined = stream
    for member in range(top_count):
        chosen = jnp.take(returned, own_slots[:, member], axis=0).astype(jnp.float32)
        combined = combined + own_weights[:, member : member + 1] * chosen
    return combined.astype(jnp.bfloat16)


def flipped(index, mask):
    bit = 1
    while bit <= mask:
        if mask & bit:
            index = index + bit * (1 - 2 * ((index // bit) % 2))
        bit *= 2
    return index


def layer_kernel(
    experts_n, columns, capacity,
    residual_ref, value_ref, gate_ref, seg_ref, conv_w_ref, gain_ref, shift_ref, ow_hbm, ffn_ref,
    slots_t_ref, slots_ref, route_w_ref, wg_ref, wu_ref, wd_ref,
    out_ref,
    ow, wg_in, wu_in, wd_in, rim, seg_ext, ext, conv_out, conv_in, stream, normed,
    outgoing, arrived, hidden, results, returned,
    ow_sem, y_send, y_recv, c_send, c_recv, f_send, f_recv, rim_send, rim_recv,
    x_send, x_recv, d_send, d_recv, r_send, r_recv,
):
    me_s, me_t = lax.axis_index("sp"), lax.axis_index("tp")
    tok_dev, local = value_ref.shape
    width = residual_ref.shape[1]
    rows_own = tok_dev // columns
    taps = conv_w_ref.shape[0]
    next_s = (me_s + 1) % experts_n
    previous_s = (me_s + experts_n - 1) % experts_n
    tile = 512

    ow_copy = pltpu.make_async_copy(ow_hbm, ow, ow_sem)
    ow_copy.start()

    def tp_peer(mask):
        return (me_s, flipped(me_t, mask))

    def sp_peer(mask):
        return (flipped(me_s, mask), me_t)

    barrier = pltpu.get_barrier_semaphore()
    peers = [tp_peer(mask) for mask in range(1, columns)]
    peers += [sp_peer(mask) for mask in range(1, experts_n)]
    for peer in peers:
        pl.semaphore_signal(barrier, inc=1, device_id=peer, device_id_type=MESH)
    pl.semaphore_wait(barrier, len(peers))

    def remote(src, dst, send, recv, peer):
        return pltpu.make_async_remote_copy(
            src_ref=src, dst_ref=dst, send_sem=send, recv_sem=recv,
            device_id=peer, device_id_type=MESH,
        )

    rim_copies = [
        remote(ref.at[pl.ds(tok_dev - RIM, RIM)], dst, rim_send.at[i], rim_recv.at[i], (next_s, me_t))
        for i, (ref, dst) in enumerate(
            ((value_ref, rim.at[0]), (gate_ref, rim.at[1]), (seg_ref, seg_ext.at[pl.ds(0, RIM)]))
        )
    ]
    for copy in rim_copies:
        copy.start()

    half = width // 2
    pieces = (
        (wg_ref, wg_in, 0, half), (wg_ref, wg_in, half, half),
        (wu_ref, wu_in, 0, width), (wd_ref, wd_in, 0, local),
    )
    across = [
        remote(own.at[pl.ds(row, n)], into.at[1, pl.ds(row, n)], y_send.at[i], y_recv.at[i], tp_peer(2))
        for i, (own, into, row, n) in enumerate(pieces)
    ]
    forward = [
        remote(into.at[1, pl.ds(row, n)], into.at[2, pl.ds(row, n)], f_send.at[i], f_recv.at[i], tp_peer(1))
        for i, (own, into, row, n) in enumerate(pieces)
    ]
    beside = [
        remote(own, into.at[0], c_send.at[i], c_recv.at[i], tp_peer(1))
        for i, (own, into) in enumerate(((wg_ref, wg_in), (wu_ref, wu_in), (wd_ref, wd_in)))
    ]
    across[0].start()

    def gated_of(value, gate):
        value, gate = value.astype(jnp.float32), gate.astype(jnp.float32)
        product = value * (1.0 / (1.0 + jnp.exp(-gate)))
        return product.astype(jnp.bfloat16).astype(jnp.float32)

    def gate_rows(i, carry):
        row = pl.multiple_of(i * 64, 64)
        ext[pl.ds(row + RIM, 64), :] = gated_of(value_ref[pl.ds(row, 64), :], gate_ref[pl.ds(row, 64), :])
        seg_ext[pl.ds(row + RIM, 64), :] = seg_ref[pl.ds(row, 64), :]
        return carry

    lax.fori_loop(0, tok_dev // 64, gate_rows, 0)
    for copy in rim_copies:
        copy.wait_recv()
    ext[pl.ds(0, RIM), :] = gated_of(rim[0], rim[1])
    seg_ext[pl.ds(0, RIM), :] = jnp.where(me_s == 0, -1, seg_ext[pl.ds(0, RIM), :])

    group = DC // CONV_GROUPS
    block = 64
    lead = RIM - (taps - 1)
    for row in range(0, tok_dev, block):
        own_seg = seg_ref[row : row + block, :]
        sums = [jnp.zeros((block, group), jnp.float32) for _ in range(local // group)]
        for tap in range(taps):
            at = row + lead + tap
            same_doc = seg_ext[at : at + block, :] == own_seg
            for g in range(local // group):
                lanes = slice(g * group, (g + 1) * group)
                term = ext[at : at + block, lanes] * conv_w_ref[tap : tap + 1, lanes]
                sums[g] = sums[g] + jnp.where(same_doc, term, 0.0)
        for g in range(local // group):
            lanes = slice(g * group, (g + 1) * group)
            mean = jnp.mean(sums[g], axis=-1, keepdims=True)
            centred = sums[g] - mean
            deviation = jnp.mean(centred * centred, axis=-1, keepdims=True)
            scaled = centred * lax.rsqrt(deviation + 1e-05) * gain_ref[:, lanes] + shift_ref[:, lanes]
            conv_out[row : row + block, lanes] = (scaled / (1.0 + jnp.exp(-scaled))).astype(jnp.bfloat16)

    exchange = {}
    for mask in (3, 2, 1):
        peer_rows = pl.ds(pl.multiple_of(flipped(me_t, mask) * rows_own, rows_own), rows_own)
        exchange[mask] = remote(
            conv_out.at[peer_rows], conv_in.at[mask], x_send.at[mask], x_recv.at[mask], tp_peer(mask)
        )
        exchange[mask].start()
    for copy in across[1:] + beside:
        copy.start()
    conv_in[0] = conv_out[pl.ds(pl.multiple_of(me_t * rows_own, rows_own), rows_own), :]
    ow_copy.wait()
    for mask in (1, 2, 3):
        exchange[mask].wait_recv()

    squares = jnp.zeros((rows_own, 1), jnp.float32)
    for col in range(0, width, tile):
        cols = slice(col, col + tile)
        mixed = jnp.zeros((rows_own, tile), jnp.float32)
        for mask in range(columns):
            w_rows = pl.ds(pl.multiple_of(flipped(me_t, mask) * local, local), local)
            mixed = mixed + jnp.dot(conv_in[mask], ow[w_rows, cols], preferred_element_type=jnp.float32)
        part = residual_ref[:, cols].astype(jnp.float32) + mixed.astype(jnp.bfloat16).astype(jnp.float32)
        stream[:, cols] = part
        squares = squares + jnp.sum(part * part, axis=-1, keepdims=True)
    scale = lax.rsqrt(squares / width + 1e-06)
    normed[...] = (stream[...] * scale * ffn_ref[...]).astype(jnp.bfloat16)

    dispatch = [
        None if mask == 0 else remote(
            outgoing.at[pl.ds(mask * capacity, capacity)], arrived.at[pl.ds(mask * capacity, capacity)],
            d_send.at[mask], d_recv.at[mask], sp_peer(mask),
        )
        for mask in range(experts_n)
    ]
    half_slots = experts_n * capacity // 2
    for part in (1, 0):
        first = part * half_slots
        numbers = lax.broadcasted_iota(jnp.int32, (half_slots, rows_own), 0) + first
        picks = jnp.where(numbers == slots_t_ref[0:1, :], 1.0, 0.0)
        for member in range(1, slots_t_ref.shape[0]):
            picks = picks + jnp.where(numbers == slots_t_ref[member : member + 1, :], 1.0, 0.0)
        picks = picks.astype(jnp.bfloat16)
        for col in range(0, width, tile):
            cols = slice(col, col + tile)
            outgoing[first : first + half_slots, cols] = jnp.dot(
                picks, normed[:, cols], preferred_element_type=jnp.float32
            ).astype(jnp.bfloat16)
        for mask in reversed(range(part * experts_n // 2, (part + 1) * experts_n // 2)):
            if mask:
                dispatch[mask].start()
    arrived[0:capacity, :] = outgoing[0:capacity, :]

    near, far = slice(0, half_slots), slice(half_slots, 2 * half_slots)

    def hidden_units(mask, rows):
        g = wg_ref[...] if mask == 0 else wg_in[mask - 1]
        u = wu_ref[...] if mask == 0 else wu_in[mask - 1]
        gate_act = jnp.dot(arrived[rows, :], g, preferred_element_type=jnp.float32)
        up_act = jnp.dot(arrived[rows, :], u, preferred_element_type=jnp.float32)
        hidden[mask, rows, :] = (gate_act / (1.0 + jnp.exp(-gate_act)) * up_act).astype(jnp.bfloat16)

    for copy in beside:
        copy.wait_recv()
    for i in (0, 1):
        across[i].wait_recv()
        forward[i].start()
    for mask in range(1, experts_n // 2):
        dispatch[mask].wait_recv()
    hidden_units(0, near)
    hidden_units(1, near)
    across[2].wait_recv()
    forward[2].start()
    hidden_units(2, near)
    for i in (0, 1, 2):
        forward[i].wait_recv()
    hidden_units(3, near)
    for mask in range(experts_n // 2, experts_n):
        dispatch[mask].wait_recv()
    for mask in range(columns):
        hidden_units(mask, far)
    across[3].wait_recv()
    forward[3].start()
    forward[3].wait_recv()

    give_back = [
        None if mask == 0 else remote(
            results.at[pl.ds(mask * capacity, capacity)], returned.at[pl.ds(mask * capacity, capacity)],
            r_send.at[mask], r_recv.at[mask], sp_peer(mask),
        )
        for mask in range(experts_n)
    ]
    for part in (1, 0):
        rows = (near, far)[part]
        for col in range(0, width, tile):
            cols = slice(col, col + tile)
            total = jnp.dot(hidden[0, rows, :], wd_ref[:, cols], preferred_element_type=jnp.float32)
            for mask in range(1, columns):
                total = total + jnp.dot(
                    hidden[mask, rows, :], wd_in[mask - 1, :, cols], preferred_element_type=jnp.float32
                )
            results[rows, cols] = total.astype(jnp.bfloat16)
        for mask in reversed(range(part * experts_n // 2, (part + 1) * experts_n // 2)):
            if mask:
                give_back[mask].start()
    returned[0:capacity, :] = results[0:capacity, :]

    for mask in range(1, experts_n):
        give_back[mask].wait_recv()
    places = lax.broadcasted_iota(jnp.int32, (rows_own, experts_n * capacity), 1)
    tables = [
        jnp.where(places == slots_ref[:, m : m + 1], 1.0, 0.0).astype(jnp.bfloat16)
        for m in range(slots_ref.shape[1])
    ]
    for col in range(0, width, tile):
        cols = slice(col, col + tile)
        total = stream[:, cols]
        for m, table in enumerate(tables):
            chosen = jnp.dot(table, returned[:, cols], preferred_element_type=jnp.float32)
            total = total + route_w_ref[:, m : m + 1] * chosen
        out_ref[:, cols] = total.astype(jnp.bfloat16)

    for copy in rim_copies + across + forward + beside + list(exchange.values()):
        copy.wait_send()
    for mask in range(1, experts_n):
        dispatch[mask].wait_send()
        give_back[mask].wait_send()


def shards(*args):
    (residual, conv_value, conv_gate, segments, conv_weight, norm_gain, norm_shift, out_weight,
     ffn_gain, routes, route_weights, w_gate, w_up, w_down) = args
    tok_dev, local = conv_value.shape
    width = residual.shape[1]
    experts_n, columns = lax.axis_size("sp"), lax.axis_size("tp")
    top_count = routes.shape[1]
    capacity = max(2, 2 * tok_dev * top_count // (columns * experts_n))
    if capacity % 16 or columns != 4 or experts_n & (experts_n - 1):
        return plain_shards(*args)
    rows_own = tok_dev // columns
    first = lax.axis_index("tp") * rows_own
    own_routes = lax.dynamic_slice_in_dim(routes, first, rows_own, 0) ^ lax.axis_index("sp")
    own_weights = lax.dynamic_slice_in_dim(route_weights, first, rows_own, 0)
    slots = slot_numbers(own_routes, capacity, experts_n)
    lanes = DC // CONV_GROUPS
    slot_total = experts_n * capacity
    bf16, f32 = jnp.bfloat16, jnp.float32
    vmem, dma = pltpu.VMEM, pltpu.SemaphoreType.DMA
    spec = pl.BlockSpec(memory_space=pltpu.VMEM)
    specs = [spec] * 15
    specs[7] = pl.BlockSpec(memory_space=pl.ANY)
    return pl.pallas_call(
        functools.partial(layer_kernel, experts_n, columns, capacity),
        out_shape=jax.ShapeDtypeStruct((rows_own, width), bf16),
        in_specs=specs,
        out_specs=spec,
        scratch_shapes=[
            vmem(out_weight.shape, bf16),
            vmem((3, width, local), bf16), vmem((3, width, local), bf16), vmem((3, local, width), bf16),
            vmem((2, RIM, local), bf16), vmem((RIM + tok_dev, lanes), jnp.int32),
            vmem((RIM + tok_dev, local), f32), vmem((tok_dev, local), bf16),
            vmem((columns, rows_own, local), bf16), vmem((rows_own, width), f32),
            vmem((rows_own, width), bf16), vmem((slot_total, width), bf16),
            vmem((slot_total, width), bf16), vmem((columns, slot_total, local), bf16),
            vmem((slot_total, width), bf16), vmem((slot_total, width), bf16),
            dma, dma((4,)), dma((4,)), dma((3,)), dma((3,)), dma((4,)), dma((4,)), dma((3,)), dma((3,)),
            dma((4,)), dma((4,)), dma((experts_n,)), dma((experts_n,)), dma((experts_n,)), dma((experts_n,)),
        ],
        compiler_params=pltpu.CompilerParams(
            collective_id=0, has_side_effects=True, vmem_limit_bytes=60 * 1024 * 1024
        ),
    )(
        residual, conv_value, conv_gate,
        jnp.broadcast_to(segments[:, None], (tok_dev, lanes)), conv_weight,
        norm_gain[None], norm_shift[None], out_weight, ffn_gain[None],
        slots.T, slots, own_weights, w_gate[0], w_up[0], w_down[0],
    )


def solution(mesh):
    return jax.shard_map(
        shards,
        mesh=mesh,
        in_specs=(
            P(("sp", "tp"), None),
            P("sp", "tp"),
            P("sp", "tp"),
            P("sp"),
            P(None, "tp"),
            P("tp"),
            P("tp"),
            P(),
            P(),
            P("sp", None),
            P("sp", None),
            P("sp", None, "tp"),
            P("sp", None, "tp"),
            P("sp", "tp", None),
        ),
        out_specs=P(("sp", "tp"), None),
        check_vma=False,
    )
```

```python
import functools

import jax
import jax.numpy as jnp
from jax import lax
from jax.experimental import pallas as pl
from jax.experimental.pallas import tpu as pltpu
from jax.sharding import PartitionSpec as P

DC = 1024
CONV_GROUPS = 8
MESH = pl.DeviceIdType.MESH
RIM = 32


def passed_along(value, axis, steps):
    count = lax.axis_size(axis)
    initial, last = (max(0, -steps), min(count, count - steps))
    return lax.ppermute(value, axis, [(source, source + steps) for source in range(initial, last)])


def slot_numbers(block_routes, capacity, experts_n):
    route_pairs = block_routes.reshape(block_routes.shape[:-2] + (-1,))
    onehot = (route_pairs[..., None] == jnp.arange(experts_n, dtype=jnp.int32)).astype(jnp.int32)
    slot_rank = jnp.sum((jnp.cumsum(onehot, axis=-2) - onehot) * onehot, axis=-1)
    return (route_pairs * capacity + slot_rank).reshape(block_routes.shape)


def dispatch_matrix(slot_ids, slot_total):
    numbers = jnp.arange(slot_total, dtype=jnp.int32)[:, None, None]
    matches = jnp.any(numbers == slot_ids[..., None, :, :], axis=-1)
    return matches.astype(jnp.bfloat16)


def plain_shards(
    residual,
    conv_value,
    conv_gate,
    segments,
    conv_weight,
    norm_gain,
    norm_shift,
    out_weight,
    ffn_gain,
    routes,
    route_weights,
    w_gate,
    w_up,
    w_down,
):
    tok_dev, local_channels = conv_value.shape
    reach = conv_weight.shape[0] - 1
    whole_gate, whole_up = (
        lax.all_gather(w_gate[0], "tp", axis=1, tiled=True),
        lax.all_gather(w_up[0], "tp", axis=1, tiled=True),
    )
    whole_down = lax.all_gather(w_down[0], "tp", axis=0, tiled=True)
    gated = (conv_value.astype(jnp.float32) * jax.nn.sigmoid(conv_gate.astype(jnp.float32))).astype(
        jnp.bfloat16
    )
    rim_prev, seg_prev = passed_along(
        (gated[tok_dev - reach :], segments[tok_dev - reach :]), "sp", 1
    )
    extended = jnp.concatenate([rim_prev, gated], 0).astype(jnp.float32)
    seg_ext = jnp.concatenate([seg_prev, segments], 0)
    convolved = jnp.zeros((tok_dev, local_channels), jnp.float32)
    for offset in range(reach + 1):
        same_doc = (seg_ext[offset : offset + tok_dev] == segments)[:, None]
        convolved = convolved + jnp.where(
            same_doc, extended[offset : offset + tok_dev] * conv_weight[offset], 0.0
        )
    group_size = DC // CONV_GROUPS
    grouped = convolved.reshape(tok_dev, local_channels // group_size, group_size)
    group_mean = jnp.mean(grouped, axis=-1, keepdims=True)
    group_var = jnp.mean(jnp.square(grouped - group_mean), axis=-1, keepdims=True)
    scaled = ((grouped - group_mean) * lax.rsqrt(group_var + 1e-05)).reshape(
        tok_dev, local_channels
    ) * norm_gain + norm_shift
    conv_out = jax.nn.silu(scaled).astype(jnp.bfloat16)
    columns = lax.axis_size("tp")
    column = lax.axis_index("tp")
    rows_own = tok_dev // columns
    own_conv = lax.all_to_all(conv_out, "tp", split_axis=0, concat_axis=1, tiled=True)
    mixed = jnp.dot(own_conv, out_weight, preferred_element_type=jnp.float32)
    stream = residual.astype(jnp.float32) + lax.optimization_barrier(
        mixed.astype(jnp.bfloat16)
    ).astype(jnp.float32)
    normed = (
        stream * lax.rsqrt(jnp.mean(stream * stream, axis=-1, keepdims=True) + 1e-06) * ffn_gain
    ).astype(jnp.bfloat16)
    experts_n = lax.axis_size("sp")
    top_count = routes.shape[1]
    model_width = normed.shape[1]
    capacity = max(2, 2 * tok_dev * top_count // (columns * experts_n))
    slot_total = experts_n * capacity
    own_routes = lax.dynamic_slice_in_dim(routes, column * rows_own, rows_own, 0)
    own_weights = lax.dynamic_slice_in_dim(route_weights, column * rows_own, rows_own, 0)
    own_slots = slot_numbers(own_routes, capacity, experts_n)
    routing_table = dispatch_matrix(own_slots, slot_total)
    outgoing = jnp.dot(routing_table, normed, preferred_element_type=jnp.float32).astype(
        jnp.bfloat16
    )
    outgoing = outgoing.reshape(experts_n, capacity, model_width)
    arrived = lax.all_to_all(outgoing, "sp", split_axis=0, concat_axis=1, tiled=True).reshape(
        slot_total, model_width
    )
    gate_act = jnp.dot(arrived, whole_gate, preferred_element_type=jnp.float32)
    up_act = jnp.dot(arrived, whole_up, preferred_element_type=jnp.float32)
    hidden = (jax.nn.silu(gate_act) * up_act).astype(jnp.bfloat16)
    summed = jnp.dot(hidden, whole_down, preferred_element_type=jnp.float32)
    expert_out = summed.astype(jnp.bfloat16).reshape(experts_n, capacity, model_width)
    returned = lax.all_to_all(expert_out, "sp", split_axis=0, concat_axis=0, tiled=True).reshape(
        slot_total, model_width
    )
    combined = stream
    for member in range(top_count):
        chosen = jnp.take(returned, own_slots[:, member], axis=0).astype(jnp.float32)
        combined = combined + own_weights[:, member : member + 1] * chosen
    return combined.astype(jnp.bfloat16)


def flipped(index, mask):
    bit = 1
    while bit <= mask:
        if mask & bit:
            index = index + bit * (1 - 2 * ((index // bit) % 2))
        bit *= 2
    return index


def layer_kernel(
    experts_n, columns, capacity,
    residual_ref, value_ref, gate_ref, seg_ref, conv_w_ref, gain_ref, shift_ref, ow_hbm, ffn_ref,
    routes_ref, route_w_ref, wg_ref, wu_ref, wd_ref,
    out_ref,
    ow, wg_in, wu_in, wd_in, rim, seg_ext, ext, conv_out, conv_in, stream, normed,
    outgoing, arrived, hidden, partial, results, returned, seg_in, tables,
    ow_sem, y_send, y_recv, c_send, c_recv, f_send, f_recv, rim_send, rim_recv,
    x_send, x_recv, d_send, d_recv, r_send, r_recv,
):
    me_s, me_t = lax.axis_index("sp"), lax.axis_index("tp")
    tok_dev, local = value_ref.shape
    width = residual_ref.shape[1]
    rows_own = tok_dev // columns
    taps = conv_w_ref.shape[0]
    next_s = (me_s + 1) % experts_n
    previous_s = (me_s + experts_n - 1) % experts_n
    tile = 512

    ow_copy = pltpu.make_async_copy(ow_hbm, ow, ow_sem)
    ow_copy.start()

    def tp_peer(mask):
        return (me_s, flipped(me_t, mask))

    def sp_peer(mask):
        return (flipped(me_s, mask), me_t)

    barrier = pltpu.get_barrier_semaphore()
    peers = [tp_peer(mask) for mask in range(1, columns)]
    peers += [sp_peer(mask) for mask in range(1, experts_n)]
    for peer in peers:
        pl.semaphore_signal(barrier, inc=1, device_id=peer, device_id_type=MESH)
    pl.semaphore_wait(barrier, len(peers))

    def remote(src, dst, send, recv, peer):
        return pltpu.make_async_remote_copy(
            src_ref=src, dst_ref=dst, send_sem=send, recv_sem=recv,
            device_id=peer, device_id_type=MESH,
        )

    last = pl.ds(tok_dev - RIM, RIM)
    rim_copies = [
        remote(ref, dst, rim_send.at[i], rim_recv.at[i], (next_s, me_t))
        for i, (ref, dst) in enumerate(
            ((value_ref.at[last], rim.at[0]), (gate_ref.at[last], rim.at[1]), (seg_ref, seg_in))
        )
    ]
    for copy in rim_copies:
        copy.start()

    half = width // 2
    pieces = (
        (wg_ref, wg_in, 0, half), (wg_ref, wg_in, half, half),
        (wu_ref, wu_in, 0, width), (wd_ref, wd_in, 0, local),
    )
    across = [
        remote(own.at[pl.ds(row, n)], into.at[1, pl.ds(row, n)], y_send.at[i], y_recv.at[i], tp_peer(2))
        for i, (own, into, row, n) in enumerate(pieces)
    ]
    forward = [
        remote(into.at[1, pl.ds(row, n)], into.at[2, pl.ds(row, n)], f_send.at[i], f_recv.at[i], tp_peer(1))
        for i, (own, into, row, n) in enumerate(pieces)
    ]
    beside = [
        remote(own, into.at[0], c_send.at[i], c_recv.at[i], tp_peer(1))
        for i, (own, into) in enumerate(((wg_ref, wg_in), (wu_ref, wu_in), (wd_ref, wd_in)))
    ]
    across[0].start()

    def gated_of(value, gate):
        value, gate = value.astype(jnp.float32), gate.astype(jnp.float32)
        product = value * (1.0 / (1.0 + jnp.exp(-gate)))
        return product.astype(jnp.bfloat16).astype(jnp.float32)

    def gate_rows(i, carry):
        row = pl.multiple_of(i * 64, 64)
        ext[pl.ds(row + RIM, 64), :] = gated_of(value_ref[pl.ds(row, 64), :], gate_ref[pl.ds(row, 64), :])
        return carry

    lax.fori_loop(0, tok_dev // 64, gate_rows, 0)
    lanes_n = seg_ref.shape[1]

    def column(row):
        return jnp.broadcast_to(row.astype(jnp.float32), (lanes_n, lanes_n)).T

    for i in range(seg_ref.shape[0]):
        seg_ext[RIM + i * lanes_n : RIM + (i + 1) * lanes_n, :] = column(seg_ref[i : i + 1, :])
    own_lanes = pl.ds(pl.multiple_of(me_t * rows_own, rows_own), rows_own)
    numbers = lax.broadcasted_iota(jnp.int32, (rows_own, lanes_n), 1).astype(jnp.float32)
    names = [column(routes_ref[m : m + 1, own_lanes]) for m in range(routes_ref.shape[0])]
    shares = [column(route_w_ref[m : m + 1, own_lanes])[:, 0:1] for m in range(routes_ref.shape[0])]
    marks = [jnp.where(name == numbers, 1.0, 0.0) for name in names]
    earlier = jnp.where(
        lax.broadcasted_iota(jnp.int32, (rows_own, rows_own), 0)
        > lax.broadcasted_iota(jnp.int32, (rows_own, rows_own), 1), 1.0, 0.0,
    ).astype(jnp.bfloat16)
    counts = jnp.dot(earlier, sum(marks).astype(jnp.bfloat16), preferred_element_type=jnp.float32)
    slot_places = lax.broadcasted_iota(jnp.int32, (rows_own, experts_n * capacity), 1)
    for m, mark in enumerate(marks):
        rank = jnp.sum(counts * mark, axis=-1, keepdims=True).astype(jnp.int32)
        slot = (names[m][:, 0:1].astype(jnp.int32) ^ me_s) * capacity + rank
        tables[m] = jnp.where(slot_places == slot, 1.0, 0.0).astype(jnp.bfloat16)
    for copy in rim_copies:
        copy.wait_recv()
    ext[pl.ds(0, RIM), :] = gated_of(rim[0], rim[1])
    before = column(seg_in[seg_ref.shape[0] - 1 : seg_ref.shape[0], :])[lanes_n - RIM :, :]
    seg_ext[0:RIM, :] = jnp.where(me_s == 0, -1.0, before)

    group = DC // CONV_GROUPS
    block = 64
    lead = RIM - (taps - 1)
    for row in range(0, tok_dev, block):
        own_seg = seg_ext[row + RIM : row + RIM + block, :]
        sums = [jnp.zeros((block, group), jnp.float32) for _ in range(local // group)]
        for tap in range(taps):
            at = row + lead + tap
            same_doc = seg_ext[at : at + block, :] == own_seg
            for g in range(local // group):
                lanes = slice(g * group, (g + 1) * group)
                term = ext[at : at + block, lanes] * conv_w_ref[tap : tap + 1, lanes]
                sums[g] = sums[g] + jnp.where(same_doc, term, 0.0)
        for g in range(local // group):
            lanes = slice(g * group, (g + 1) * group)
            mean = jnp.mean(sums[g], axis=-1, keepdims=True)
            centred = sums[g] - mean
            deviation = jnp.mean(centred * centred, axis=-1, keepdims=True)
            scaled = centred * lax.rsqrt(deviation + 1e-05) * gain_ref[:, lanes] + shift_ref[:, lanes]
            conv_out[row : row + block, lanes] = (scaled / (1.0 + jnp.exp(-scaled))).astype(jnp.bfloat16)

    exchange = {}
    for mask in (3, 2, 1):
        peer_rows = pl.ds(pl.multiple_of(flipped(me_t, mask) * rows_own, rows_own), rows_own)
        exchange[mask] = remote(
            conv_out.at[peer_rows], conv_in.at[mask], x_send.at[mask], x_recv.at[mask], tp_peer(mask)
        )
        exchange[mask].start()
    for copy in across[1:] + beside:
        copy.start()
    conv_in[0] = conv_out[pl.ds(pl.multiple_of(me_t * rows_own, rows_own), rows_own), :]
    ow_copy.wait()
    for mask in (1, 2, 3):
        exchange[mask].wait_recv()

    squares = jnp.zeros((rows_own, 1), jnp.float32)
    for col in range(0, width, tile):
        cols = slice(col, col + tile)
        mixed = jnp.zeros((rows_own, tile), jnp.float32)
        for mask in range(columns):
            w_rows = pl.ds(pl.multiple_of(flipped(me_t, mask) * local, local), local)
            mixed = mixed + jnp.dot(conv_in[mask], ow[w_rows, cols], preferred_element_type=jnp.float32)
        part = residual_ref[:, cols].astype(jnp.float32) + mixed.astype(jnp.bfloat16).astype(jnp.float32)
        stream[:, cols] = part
        squares = squares + jnp.sum(part * part, axis=-1, keepdims=True)
    scale = lax.rsqrt(squares / width + 1e-06)
    normed[...] = (stream[...] * scale * ffn_ref[...]).astype(jnp.bfloat16)

    dispatch = [
        None if mask == 0 else remote(
            outgoing.at[pl.ds(mask * capacity, capacity)], arrived.at[pl.ds(mask * capacity, capacity)],
            d_send.at[mask], d_recv.at[mask], sp_peer(mask),
        )
        for mask in range(experts_n)
    ]
    half_slots = experts_n * capacity // 2
    for part in (1, 0):
        first = part * half_slots
        picks = sum(
            tables[m, :, first : first + half_slots].astype(jnp.float32) for m in range(len(names))
        ).T.astype(jnp.bfloat16)
        for col in range(0, width, tile):
            cols = slice(col, col + tile)
            outgoing[first : first + half_slots, cols] = jnp.dot(
                picks, normed[:, cols], preferred_element_type=jnp.float32
            ).astype(jnp.bfloat16)
        for mask in reversed(range(part * experts_n // 2, (part + 1) * experts_n // 2)):
            if mask:
                dispatch[mask].start()
    arrived[0:capacity, :] = outgoing[0:capacity, :]

    near, far = slice(0, half_slots), slice(half_slots, 2 * half_slots)

    def hidden_units(mask, rows):
        g = wg_ref[...] if mask == 0 else wg_in[mask - 1]
        u = wu_ref[...] if mask == 0 else wu_in[mask - 1]
        gate_act = jnp.dot(arrived[rows, :], g, preferred_element_type=jnp.float32)
        up_act = jnp.dot(arrived[rows, :], u, preferred_element_type=jnp.float32)
        hidden[mask, rows, :] = (gate_act / (1.0 + jnp.exp(-gate_act)) * up_act).astype(jnp.bfloat16)

    for copy in beside:
        copy.wait_recv()
    for i in (0, 1):
        across[i].wait_recv()
        forward[i].start()
    for mask in range(1, experts_n // 2):
        dispatch[mask].wait_recv()
    hidden_units(0, near)
    hidden_units(1, near)
    across[2].wait_recv()
    forward[2].start()
    hidden_units(2, near)
    for i in (0, 1, 2):
        forward[i].wait_recv()
    hidden_units(3, near)
    for mask in range(experts_n // 2, experts_n):
        dispatch[mask].wait_recv()
    for mask in range(columns):
        hidden_units(mask, far)
    def down(mask, rows, cols):
        w = wd_ref[:, cols] if mask == 0 else wd_in[mask - 1, :, cols]
        return jnp.dot(hidden[mask, rows, :], w, preferred_element_type=jnp.float32)

    for rows in (far, near):
        for col in range(0, width, tile):
            cols = slice(col, col + tile)
            partial[rows, cols] = down(0, rows, cols) + down(1, rows, cols)
    across[3].wait_recv()
    forward[3].start()
    for col in range(0, width, tile):
        cols = slice(col, col + tile)
        partial[far, cols] += down(2, far, cols)
    forward[3].wait_recv()

    give_back = [
        None if mask == 0 else remote(
            results.at[pl.ds(mask * capacity, capacity)], returned.at[pl.ds(mask * capacity, capacity)],
            r_send.at[mask], r_recv.at[mask], sp_peer(mask),
        )
        for mask in range(experts_n)
    ]
    for part in (1, 0):
        rows = (near, far)[part]
        for col in range(0, width, tile):
            cols = slice(col, col + tile)
            total = partial[rows, cols] + down(3, rows, cols)
            if part == 0:
                total = total + down(2, rows, cols)
            results[rows, cols] = total.astype(jnp.bfloat16)
        for mask in reversed(range(part * experts_n // 2, (part + 1) * experts_n // 2)):
            if mask:
                give_back[mask].start()
    returned[0:capacity, :] = results[0:capacity, :]

    for part in (0, 1):
        rows = (near, far)[part]
        for mask in range(part * experts_n // 2, (part + 1) * experts_n // 2):
            if mask:
                give_back[mask].wait_recv()
        for col in range(0, width, tile):
            cols = slice(col, col + tile)
            total = stream[:, cols]
            for m, share in enumerate(shares):
                chosen = jnp.dot(tables[m, :, rows], returned[rows, cols], preferred_element_type=jnp.float32)
                total = total + share * chosen
            if part == 0:
                stream[:, cols] = total
            else:
                out_ref[:, cols] = total.astype(jnp.bfloat16)

    for copy in rim_copies + across + forward + beside + list(exchange.values()):
        copy.wait_send()
    for mask in range(1, experts_n):
        dispatch[mask].wait_send()
        give_back[mask].wait_send()


def shards(*args):
    (residual, conv_value, conv_gate, segments, conv_weight, norm_gain, norm_shift, out_weight,
     ffn_gain, routes, route_weights, w_gate, w_up, w_down) = args
    tok_dev, local = conv_value.shape
    width = residual.shape[1]
    experts_n, columns = lax.axis_size("sp"), lax.axis_size("tp")
    top_count = routes.shape[1]
    capacity = max(2, 2 * tok_dev * top_count // (columns * experts_n))
    if capacity % 32 or columns != 4 or tok_dev != columns * 128 or experts_n & (experts_n - 1):
        return plain_shards(*args)
    rows_own = tok_dev // columns
    lanes = DC // CONV_GROUPS
    slot_total = experts_n * capacity
    bf16, f32 = jnp.bfloat16, jnp.float32
    vmem, dma = pltpu.VMEM, pltpu.SemaphoreType.DMA
    spec = pl.BlockSpec(memory_space=pltpu.VMEM)
    specs = [spec] * 14
    specs[7] = pl.BlockSpec(memory_space=pl.ANY)
    return pl.pallas_call(
        functools.partial(layer_kernel, experts_n, columns, capacity),
        out_shape=jax.ShapeDtypeStruct((rows_own, width), bf16),
        in_specs=specs,
        out_specs=spec,
        scratch_shapes=[
            vmem(out_weight.shape, bf16),
            vmem((3, width, local), bf16), vmem((3, width, local), bf16), vmem((3, local, width), bf16),
            vmem((2, RIM, local), bf16), vmem((RIM + tok_dev, lanes), f32),
            vmem((RIM + tok_dev, local), f32), vmem((tok_dev, local), bf16),
            vmem((columns, rows_own, local), bf16), vmem((rows_own, width), f32),
            vmem((rows_own, width), bf16), vmem((slot_total, width), bf16),
            vmem((slot_total, width), bf16), vmem((columns, slot_total, local), bf16),
            vmem((slot_total, width), f32),
            vmem((slot_total, width), bf16), vmem((slot_total, width), bf16),
            vmem((tok_dev // lanes, lanes), jnp.int32), vmem((top_count, rows_own, slot_total), bf16),
            dma, dma((4,)), dma((4,)), dma((3,)), dma((3,)), dma((4,)), dma((4,)), dma((3,)), dma((3,)),
            dma((4,)), dma((4,)), dma((experts_n,)), dma((experts_n,)), dma((experts_n,)), dma((experts_n,)),
        ],
        compiler_params=pltpu.CompilerParams(
            collective_id=0, has_side_effects=True, vmem_limit_bytes=60 * 1024 * 1024
        ),
    )(
        residual, conv_value, conv_gate,
        segments.reshape(-1, lanes), conv_weight,
        norm_gain[None], norm_shift[None], out_weight, ffn_gain[None],
        routes.T, route_weights.T, w_gate[0], w_up[0], w_down[0],
    )


def solution(mesh):
    return jax.shard_map(
        shards,
        mesh=mesh,
        in_specs=(
            P(("sp", "tp"), None),
            P("sp", "tp"),
            P("sp", "tp"),
            P("sp"),
            P(None, "tp"),
            P("tp"),
            P("tp"),
            P(),
            P(),
            P("sp", None),
            P("sp", None),
            P("sp", None, "tp"),
            P("sp", None, "tp"),
            P("sp", "tp", None),
        ),
        out_specs=P(("sp", "tp"), None),
        check_vma=False,
    )
```
